32 devices in a mesh: ep: 8 (over z, core), tp: 4 (over y, x).
Axes of the slice: x: 2, y: 2, z: 4, core: 2. Of those that a mesh axis runs over, the one named last changes fastest.
Arguments:
- branch_in: bfloat16 [8192, 512], P(('ep', 'tp')), may hold values from -6 to 6
- pool_weight: bfloat16 [4, 128, 128], replicated, may hold values from -0.5 to 0.5
- group_gain: float32 [512], replicated, may hold values from 0.1 to 1.9
- out_weight: bfloat16 [512, 2048], P(None, 'tp'), may hold values from -0.25 to 0.25
- out_gain: float32 [2048], replicated, may hold values from 0.1 to 1.9
- ffn_input: bfloat16 [1024, 2048], P('ep'), may hold values from -6 to 6
- ffn_gain: float32 [2048], replicated, may hold values from 0.1 to 1.9
- routes: int32 [1024, 4], P('ep'), may hold values from 0 to 7, all different within a row; in each aligned block of 128 rows (0 to 127, 128 to 255, ...) at most 128 rows name the same one
- route_weight: float32 [1024, 4], P('ep'), may hold values from 0.2 to 2
- gate_weight: bfloat16 [8, 2048, 4096], P('ep', None, 'tp'), may hold values from -0.375 to 0.375
- up_weight: bfloat16 [8, 2048, 4096], P('ep', None, 'tp'), may hold values from -0.375 to 0.375
- down_weight: bfloat16 [8, 4096, 2048], P('ep', 'tp'), may hold values from -0.0078125 to 0.0078125
Outputs:
- mixer_out: bfloat16 [8192, 2048], P(('ep', 'tp'))
- expert_out: bfloat16 [1024, 2048], P('ep', 'tp')
The draws below stay inside these ranges and needn't reach their ends.
Inputs may be any that keep to these rules, and one draw needn't show every extreme that they name: `routes`: each row names 4 different experts. Among the 128 rows of one index of ep no expert is named by more than 128 rows, and in some such block one expert is named by exactly 128.
All inputs are finite; a program needn't handle non-finite values.
Results may differ from the reference program's by a relative error of at most 0.017.
Values may be sent and summed in bfloat16 or wider, within the bound.
A program may use at most 64 MiB of HBM per device.

```python
import math
import jax
import jax.numpy as jnp
import numpy as np
from jax import lax

D = 2048
POOL_CH = 128
GW = 512
FF = 4096
TOPK = 4
RA = 256
RB = 128
EXPERTS = 8
CAP = 128
TOKENS_A = 8192
TOKENS_B = 1024
N_EP = 8
N_TP = 4


def block_scale(rng, dims, split, least, largest):
    level = 1.0
    for axis_at, blocks in split:
        draws = jax.random.uniform(jax.random.fold_in(jax.random.fold_in(rng, 6), axis_at), (blocks,), jnp.float32, least / len(split), largest / len(split))
        level = level * jnp.repeat(jnp.exp(draws), dims[axis_at] // blocks).reshape((-1,) + (1,) * (len(dims) - 1 - axis_at))
    return level


def routed_block(stream_key, own, number, rows, amount, top, most, lean):
    ranking = jax.random.permutation(stream_key, amount)
    heavy_load, usual = shares(amount, rows * top, most, lean, True), shares(amount, rows * top, most, lean, False)
    places = jnp.arange(amount)

    def named(lengths, rotation):
        used = int((lengths > 0).sum())
        fixed = max(1, used // 4)
        passed = fixed + (places - fixed + rotation * (used - fixed)) % max(1, amount - fixed)
        return jnp.zeros((amount,), jnp.int32).at[ranking[jnp.where(places < fixed, places, passed)]].set(jnp.asarray(lengths, jnp.int32))

    lengths = jnp.where(number % 4 == 0, named(heavy_load, number // 4), named(usual, number - number // 4 - 1))
    mixed = jax.random.permutation(jax.random.fold_in(own, 3), amount)
    source_of, receiver = mixed[0:amount // 2 * 2:2], mixed[1:amount // 2 * 2:2]
    room = jnp.minimum(lengths[source_of] - 1, most - lengths[receiver]) // 2
    room = jnp.where((source_of == ranking[0]) | (receiver == ranking[0]) | (lengths[receiver] == 0), 0, jnp.maximum(room, 0))
    passed = jax.random.randint(jax.random.fold_in(own, 4), (amount // 2,), 0, 1 << 20) % (room + 1)
    lengths = lengths.at[source_of].add(-passed).at[receiver].add(passed)
    labels = jnp.searchsorted(jnp.cumsum(lengths), jnp.arange(rows * top), side="right").astype(jnp.int32)
    listing = labels.reshape(top, rows).T
    listing = listing[jax.random.permutation(jax.random.fold_in(own, 1), rows)]
    rotation = jax.random.randint(jax.random.fold_in(own, 2), (rows, 1), 0, top)
    return jnp.take_along_axis(listing, (jnp.arange(top)[None, :] + rotation) % top, axis=1)


def shares(number_of, total, limit, skew, full):
    loads = [(1 << 20) // math.isqrt(standing ** skew) + 1 for standing in range(1, number_of + 1)]
    largest = limit if full else min(limit, max(-(-total // number_of), total * loads[0] // sum(loads)))
    least = 1 if total - largest >= number_of - 1 else 0
    holding, rest = [largest] + [least] * (number_of - 1), total - largest - least * (number_of - 1)
    while rest > 0:
        candidates = [i for i in range(1, number_of) if holding[i] < largest] or [i for i in range(1, number_of) if holding[i] < limit]
        pool, remaining = sum([loads[i] for i in candidates]), rest
        for i in candidates:
            addition = min(limit - holding[i], max(1, remaining * loads[i] // pool), rest)
            holding[i] = holding[i] + addition
            rest = rest - addition
    return np.array(holding)


def scatter_about(stream_key, dims, spread, limit, pieces=(), held_as=jnp.bfloat16):
    result = jax.random.normal(stream_key, dims, jnp.float32) * spread
    if len(pieces) > 0:
        result = block_scale(stream_key, dims, pieces, -0.22, 0.18) * result
    return jnp.clip(result, min=-limit, max=limit).astype(held_as)


def setup_inputs(seed: int = 0) -> dict:
    keys = jax.random.split(jax.random.key(seed), 13)
    branch_in = scatter_about(keys[0], (TOKENS_A, GW), 1.0, 6.0, ((0, 32),))
    pool_weight = scatter_about(keys[1], (4, POOL_CH, POOL_CH), POOL_CH ** -0.5, 0.5)
    group_gain = jnp.clip(1.0 + 0.18 * jax.random.normal(keys[2], (GW,), jnp.float32), 0.1, 1.9)
    out_weight = scatter_about(keys[3], (GW, D), GW ** -0.5, 0.25, ((1, 4),))
    out_gain = jnp.clip(1.0 + 0.18 * jax.random.normal(keys[4], (D,), jnp.float32), 0.1, 1.9)
    ffn_input = scatter_about(keys[5], (TOKENS_B, D), 1.0, 6.0, ((0, 8),))
    ffn_gain = jnp.clip(1.0 + 0.18 * jax.random.normal(keys[6], (D,), jnp.float32), 0.1, 1.9)
    routes_keys = jax.random.split(jax.random.fold_in(keys[7], 1), TOKENS_B // RB)
    routes_turns = jax.random.permutation(jax.random.fold_in(keys[7], 3), TOKENS_B // RB)
    routes = jax.vmap(lambda own, number: routed_block(jax.random.fold_in(keys[7], 2), own, number, RB, EXPERTS, TOPK, CAP, 2))(routes_keys, routes_turns).reshape((TOKENS_B, TOPK))
    route_weight = jnp.clip(jnp.exp(math.log(2.0) - 2.3025851 * jax.random.uniform(keys[8], (TOKENS_B, TOPK), jnp.float32) ** block_scale(keys[8], (TOKENS_B, TOPK), ((0, 8),), -0.2, 0.2)), 0.2, 2.0)
    gate_weight = scatter_about(keys[9], (EXPERTS, D, FF), (D // 9) ** -0.5, 0.375, ((0, 8), (2, 4)))
    up_weight = scatter_about(keys[10], (EXPERTS, D, FF), (D // 9) ** -0.5, 0.375, ((0, 8), (2, 4)))
    down_weight = scatter_about(keys[11], (EXPERTS, FF, D), (FF * 160) ** -0.5, 0.0078125, ((0, 8), (1, 4)))
    return dict(branch_in=branch_in, pool_weight=pool_weight, group_gain=group_gain, out_weight=out_weight, out_gain=out_gain, ffn_input=ffn_input, ffn_gain=ffn_gain, routes=routes, route_weight=route_weight, gate_weight=gate_weight, up_weight=up_weight, down_weight=down_weight)


pool_windows = (2, 4, 8, 16)
rim_rows = 15
norm_eps = 1e-06
clamp_limit = 7.0
sigmoid_slope = 1.702

def rms_scale(values, gain):
    return values * lax.rsqrt(lax.optimization_barrier(jnp.mean(values * values, axis=-1, keepdims=True)) + norm_eps) * gain.astype(jnp.float32)

def slot_tables(route_block, expert_count, capacity):
    row_count, top_count = route_block.shape
    flat_experts = route_block.reshape(-1)
    one_hot = (flat_experts[:, None] == jnp.arange(expert_count, dtype=jnp.int32)[None, :]).astype(jnp.int32)
    earlier = jnp.cumsum(one_hot, axis=0) - one_hot
    slot_index = lax.optimization_barrier(jnp.sum(earlier * one_hot, axis=1))
    flat_slots = (slot_index * expert_count + flat_experts).astype(jnp.int32)
    owner_rows = jnp.full((capacity * expert_count,), row_count, jnp.int32)
    owner_rows = owner_rows.at[flat_slots].set(jnp.arange(row_count * top_count, dtype=jnp.int32) // top_count)
    return (flat_slots, owner_rows)

def pool_reference(branch_in, pool_weight, group_gain, out_weight, out_gain):
    total_rows, width = branch_in.shape
    group_chans = width // len(pool_windows)
    widened = jnp.concatenate([jnp.zeros((rim_rows, width), jnp.bfloat16), branch_in], axis=0)
    window = jnp.repeat(jnp.array(pool_windows, jnp.int32), group_chans)

    def one_block(block_index):
        first_row = (block_index * RA).astype(jnp.int32)
        segment = lax.dynamic_slice_in_dim(widened, first_row, RA + rim_rows, 0).astype(jnp.float32)
        positions = first_row + jnp.arange(RA, dtype=jnp.int32)
        summed = jnp.zeros((RA, width), jnp.float32)
        for offset_back in range(rim_rows + 1):
            shifted = segment[rim_rows - offset_back:rim_rows - offset_back + RA]
            summed = summed + jnp.where(window[None, :] > offset_back, shifted, jnp.float32(0.0))
        counts = jnp.minimum(window[None, :], positions[:, None] + 1).astype(jnp.float32)
        pooled = (summed / counts - segment[rim_rows:]).astype(jnp.bfloat16)
        mixed_parts = []
        for group_index in range(len(pool_windows)):
            lower = group_index * group_chans
            mixed_parts.append(jnp.dot(pooled[:, lower:lower + group_chans], pool_weight[group_index], preferred_element_type=jnp.float32))
        group_mix = jnp.concatenate(mixed_parts, axis=1)
        mixed_rows = rms_scale(group_mix, group_gain).astype(jnp.bfloat16)
        projected = jnp.dot(mixed_rows, out_weight, preferred_element_type=jnp.float32)
        return rms_scale(projected, out_gain).astype(jnp.bfloat16)
    blocks = lax.map(one_block, jnp.arange(total_rows // RA, dtype=jnp.int32))
    return blocks.reshape(total_rows, out_weight.shape[1])

def expert_reference(ffn_input, ffn_gain, routes, route_weight, gate_weight, up_weight, down_weight):
    total_rows, model_width = ffn_input.shape
    top_count = routes.shape[1]
    expert_count = gate_weight.shape[0]
    hidden_width = gate_weight.shape[2]
    row_count = total_rows // N_EP
    capacity = 2 * row_count * top_count // expert_count
    normed_rows = rms_scale(ffn_input.astype(jnp.float32), ffn_gain).astype(jnp.bfloat16)
    route_blocks = routes.reshape(N_EP, row_count, top_count)
    flat_slots, owner_rows = jax.vmap(lambda route_block: slot_tables(route_block, expert_count, capacity))(route_blocks)
    padded = jnp.concatenate([normed_rows.reshape(N_EP, row_count, model_width), jnp.zeros((N_EP, 1, model_width), jnp.bfloat16)], axis=1)
    slot_rows = jax.vmap(lambda block_rows, block_owner: block_rows[block_owner])(padded, owner_rows)
    slot_rows = slot_rows.reshape(N_EP, capacity, expert_count, model_width)
    by_expert = jnp.moveaxis(slot_rows, 2, 0).reshape(expert_count, N_EP * capacity, model_width)

    def one_expert(operands):
        expert_rows, gate_local, up_local, down_local = operands
        gate_pre = jnp.minimum(jnp.dot(expert_rows, gate_local, preferred_element_type=jnp.float32), clamp_limit)
        up_pre = jnp.clip(jnp.dot(expert_rows, up_local, preferred_element_type=jnp.float32), -clamp_limit, clamp_limit)
        hidden = ((up_pre + 1.0) * gate_pre * jax.nn.sigmoid(sigmoid_slope * gate_pre)).astype(jnp.bfloat16)
        block_width = hidden_width // N_TP
        part_hidden = hidden.astype(jnp.float32).reshape(expert_rows.shape[0], N_TP, block_width)
        part_down = down_local.astype(jnp.float32).reshape(N_TP, block_width, model_width)
        partials = jnp.einsum('ntf,tfd->tnd', part_hidden, part_down)
        partials = partials.astype(jnp.bfloat16).astype(jnp.float32)
        return lax.optimization_barrier(jnp.sum(partials, axis=0)).astype(jnp.bfloat16)
    results = lax.map(one_expert, (by_expert, gate_weight, up_weight, down_weight))
    results = results.reshape(expert_count, N_EP, capacity, model_width).transpose(1, 2, 0, 3)
    results = results.reshape(N_EP, capacity * expert_count, model_width)
    picked = jax.vmap(lambda block_results, block_slots: block_results[block_slots])(results, flat_slots)
    picked = picked.reshape(total_rows, top_count, model_width).astype(jnp.float32)
    return lax.optimization_barrier(jnp.sum(picked * route_weight[:, :, None], axis=1)).astype(jnp.bfloat16)

def reference(branch_in, pool_weight, group_gain, out_weight, out_gain, ffn_input, ffn_gain, routes, route_weight, gate_weight, up_weight, down_weight):
    mixer_out = pool_reference(branch_in, pool_weight, group_gain, out_weight, out_gain)
    expert_out = expert_reference(ffn_input, ffn_gain, routes, route_weight, gate_weight, up_weight, down_weight)
    return (mixer_out, expert_out)
```

```python
import functools
import jax
import jax.numpy as jnp
from jax import lax
from jax.experimental import pallas as pl
from jax.experimental.pallas import tpu as pltpu
from jax.sharding import PartitionSpec as P

pool_windows = (2, 4, 8, 16)
rim_rows = 16
norm_eps = 1e-06
clamp_limit = 7.0
sigmoid_slope = 1.702
MESH = pl.DeviceIdType.MESH
f32 = jnp.float32
bf16 = jnp.bfloat16


def rms_scale(values, gain):
    return values * lax.rsqrt(jnp.mean(values * values, axis=-1, keepdims=True) + norm_eps) * gain


def kernel(
    n_ep, n_tp,
    branch, pool_w, group_gain, out_w, out_gain, x_own, ffn_gain, w_own, gate_h, up_h, down_h,
    mixer_out, expert_out,
    gate, up, down, xg, wg, rim, ow, xn, hid, mixed, proj,
    pown, psend, precv, tsend, trecv, fsend, frecv, facc,
    local_sem, s_z, r_z, s_x, r_x, s_p, r_p, s_w, r_w, s_rim, r_rim,
    s_ow, r_ow, s_owp, r_owp, s_ps, r_ps, s_t, r_t, s_f, r_f,
):
    e = lax.axis_index("ep")
    j = lax.axis_index("tp")
    nz = n_ep // 2
    z = e // 2
    c = e % 2
    rows, width = x_own.shape
    cols = width // n_tp
    mate = z * 2 + (1 - c)
    last = (j == n_tp - 1).astype(jnp.int32)
    first = (j == 0).astype(jnp.int32)
    nxt = ((e + last) % n_ep, (j + 1) % n_tp)
    prv = ((e - first + n_ep) % n_ep, (j - 1 + n_tp) % n_tp)

    def colsl(q):
        return pl.ds(pl.multiple_of(q * cols, cols), cols)

    def remote(src, dst, ssem, rsem, ep, tp):
        return pltpu.make_async_remote_copy(
            src_ref=src, dst_ref=dst, send_sem=ssem, recv_sem=rsem,
            device_id=(ep, tp), device_id_type=MESH,
        )

    def ep_at(d):
        return (z + d) % nz * 2 + c

    def src_ep(d):
        return (z - d + nz) % nz * 2 + c

    def src_mate(d):
        return (z - d + nz) % nz * 2 + (1 - c)

    def tp_at(t):
        return (j + t) % n_tp

    loads = [
        pltpu.make_async_copy(gate_h.at[0], gate, local_sem.at[0]),
        pltpu.make_async_copy(up_h.at[0], up, local_sem.at[1]),
        pltpu.make_async_copy(down_h.at[0], down, local_sem.at[2]),
    ]
    own_copy = pltpu.make_async_copy(x_own, xg.at[e], local_sem.at[3])
    own_w = pltpu.make_async_copy(w_own, wg.at[e], local_sem.at[4])
    own_ow = pltpu.make_async_copy(out_w, ow.at[j], local_sem.at[5])
    own_copy.start()
    own_w.start()
    own_ow.start()
    for load in loads:
        load.start()

    barrier = pltpu.get_barrier_semaphore()
    for d in range(1, n_ep):
        pl.semaphore_signal(barrier, inc=1, device_id=((e + d) % n_ep, j), device_id_type=MESH)
    for t in range(1, n_tp):
        pl.semaphore_signal(barrier, inc=1, device_id=(e, tp_at(t)), device_id_type=MESH)
    pl.semaphore_signal(barrier, inc=1, device_id=nxt, device_id_type=MESH)
    pl.semaphore_signal(barrier, inc=1, device_id=prv, device_id_type=MESH)
    pl.semaphore_wait(barrier, n_ep - 1 + n_tp - 1 + 2)

    def z_copy(d):
        return remote(
            x_own.at[:, colsl(j)], xg.at[e, :, colsl(j)], s_z.at[d], r_z.at[d], ep_at(d), j
        )

    def z_arrival(d):
        view = xg.at[src_ep(d), :, colsl(j)]
        return remote(view, view, s_z.at[d], r_z.at[d], ep_at(d), j)

    def x_copy(d, t):
        view = xg.at[src_ep(d), :, colsl(j)]
        return remote(view, view, s_x.at[d, t], r_x.at[d, t], e, tp_at(t))

    def x_arrival(d, t):
        view = xg.at[src_ep(d), :, colsl(tp_at(n_tp - t))]
        return remote(view, view, s_x.at[d, t], r_x.at[d, t], e, tp_at(t))

    def p_copy(d):
        view = xg.at[src_ep(d)]
        return remote(view, view, s_p.at[d], r_p.at[d], mate, j)

    def p_arrival(d):
        view = xg.at[src_mate(d)]
        return remote(view, view, s_p.at[d], r_p.at[d], mate, j)

    own_p = remote(x_own, xg.at[e], s_p.at[0], r_p.at[0], mate, j)
    half = out_w.shape[0] // 2
    my_half = pl.ds(pl.multiple_of(c * half, half), half)
    mate_half = pl.ds(pl.multiple_of((1 - c) * half, half), half)

    def w_copy(d):
        return remote(w_own, wg.at[e], s_w.at[d], r_w.at[d], (e + d) % n_ep, j)

    def w_arrival(d):
        return remote(w_own, wg.at[(e - d + n_ep) % n_ep], s_w.at[d], r_w.at[d], (e + d) % n_ep, j)

    def ow_copy(t):
        return remote(
            out_w.at[my_half], ow.at[j, my_half], s_ow.at[t], r_ow.at[t], e, tp_at(t)
        )

    def ow_arrival(t):
        view = ow.at[tp_at(n_tp - t), my_half]
        return remote(view, view, s_ow.at[t], r_ow.at[t], e, tp_at(t))

    def owp_copy(t):
        view = ow.at[tp_at(n_tp - t), my_half]
        return remote(view, view, s_owp.at[t], r_owp.at[t], mate, j)

    def owp_arrival(t):
        view = ow.at[tp_at(n_tp - t), mate_half]
        return remote(view, view, s_owp.at[t], r_owp.at[t], mate, j)

    rim_copy = remote(
        branch.at[pl.ds(branch.shape[0] - rim_rows, rim_rows)], rim, s_rim, r_rim, nxt[0], nxt[1]
    )

    for d in range(1, nz):
        z_copy(d).start()
    own_p.start()
    rim_copy.start()
    for d in range(1, n_ep):
        w_copy(d).start()
    for t in range(1, n_tp):
        ow_copy(t).start()

    rim_copy.wait_recv()
    branch_rows = branch.shape[0]
    chans = branch.shape[1] // len(pool_windows)
    first_row = (e * n_tp + j) * branch_rows
    positions = first_row + lax.broadcasted_iota(jnp.int32, (branch_rows, 1), 0)
    total = jnp.zeros((branch_rows, 1), f32)
    for g, window in enumerate(pool_windows):
        lanes = slice(g * chans, (g + 1) * chans)
        here = branch[:, lanes].astype(f32)
        edge = jnp.where(first_row == 0, 0.0, rim[:, lanes].astype(f32))
        wide = jnp.concatenate([edge, here], axis=0)
        reach = 1
        while reach < window:
            wide = wide + pltpu.roll(wide, reach, 0)
            reach *= 2
        counts = jnp.minimum(window, positions + 1).astype(f32)
        pooled = (wide[rim_rows:] / counts - here).astype(bf16)
        part = jnp.dot(pooled, pool_w[g], preferred_element_type=f32)
        proj[:, lanes] = part
        total = total + jnp.sum(part * part, axis=-1, keepdims=True)
    scale = lax.rsqrt(total / branch.shape[1] + norm_eps)
    mixed[...] = (proj[:, : branch.shape[1]] * scale * group_gain[...]).astype(bf16)

    def forward(d):
        z_arrival(d).wait_recv()
        for t in range(1, n_tp):
            x_copy(d, t).start()

    def to_mate(d):
        for t in range(1, n_tp):
            x_arrival(d, t).wait_recv()
        p_copy(d).start()

    if nz > 1:
        forward(1)
    own_copy.wait()
    own_w.wait()
    own_ow.wait()
    for d in range(1, n_ep):
        w_arrival(d).wait_recv()
    for load in loads[:2]:
        load.wait()

    chunk = 16

    def normed(block, at):
        def one(i, _):
            r = pl.ds(pl.multiple_of(i * chunk, chunk), chunk)
            v = xg[block, r, :].astype(f32)
            out = pl.ds(pl.multiple_of(at + i * chunk, chunk), chunk)
            xn[out, :] = rms_scale(v, ffn_gain[...]).astype(bf16)
            return 0

        lax.fori_loop(0, rows // chunk, one, 0)

    diagonal = lax.broadcasted_iota(jnp.int32, (rows, rows), 0) == lax.broadcasted_iota(
        jnp.int32, (rows, rows), 1
    )

    def row_weights(block):
        line = wg[block, pl.ds(e, 1), :]
        return jnp.sum(jnp.where(diagonal, line, 0.0), axis=1, keepdims=True)

    step_f = min(256, gate.shape[1])

    def hidden_part():
        def one(n, _):
            span = pl.ds(pl.multiple_of(n * step_f, step_f), step_f)
            g = jnp.dot(xn[...], gate[:, span], preferred_element_type=f32)
            u = jnp.dot(xn[...], up[:, span], preferred_element_type=f32)
            g = jnp.minimum(g, clamp_limit)
            u = jnp.clip(u, -clamp_limit, clamp_limit)
            hid[:, span] = ((u + 1.0) * g * jax.nn.sigmoid(sigmoid_slope * g)).astype(bf16)
            return 0

        lax.fori_loop(0, gate.shape[1] // step_f, one, 0)

    step_d = min(256, width)

    def down_part(s):
        mine = row_weights(src_ep(s))
        theirs = row_weights(src_mate(s))

        def one(q, _):
            span = pl.ds(pl.multiple_of(q * step_d, step_d), step_d)
            y = jnp.dot(hid[...], down[:, span], preferred_element_type=f32)
            pown[s % 2, :, span] = y[:rows] * mine
            psend[s, :, span] = (y[rows:] * theirs).astype(bf16)
            return 0

        lax.fori_loop(0, width // step_d, one, 0)

    def mate_sum(s):
        return remote(psend.at[s], precv.at[s], s_ps.at[s], r_ps.at[s], mate, j)

    def t_copy(s, t):
        return remote(
            tsend.at[s, :, colsl(tp_at(t))], trecv.at[s, t], s_t.at[s, t], r_t.at[s, t], e, tp_at(t)
        )

    def f_copy(s):
        return remote(fsend.at[s], frecv.at[s], s_f.at[s], r_f.at[s], src_ep(s), j)

    def stage_two(s):
        mate_sum(s).wait_recv()

        def one(i, _):
            r = pl.ds(pl.multiple_of(i * chunk, chunk), chunk)
            tsend[s, r, :] = (pown[s % 2, r, :] + precv[s, r, :].astype(f32)).astype(bf16)
            return 0

        lax.fori_loop(0, rows // chunk, one, 0)
        for t in range(1, n_tp):
            t_copy(s, t).start()

    def stage_three(s):
        for t in range(1, n_tp):
            t_copy(s, t).wait_recv()
        acc = tsend[s, :, colsl(j)].astype(f32)
        for t in range(1, n_tp):
            acc = acc + trecv[s, t].astype(f32)

        @pl.when(s == 0)
        def _():
            facc[...] = acc

        @pl.when(s > 0)
        def _():
            fsend[s] = acc.astype(bf16)
            f_copy(s).start()

    def project():
        for t in range(1, n_tp):
            owp_arrival(t).wait_recv()

        def one(q, total):
            part = jnp.dot(mixed[...], ow[q], preferred_element_type=f32)
            proj[:, colsl(q)] = part
            return total + jnp.sum(part * part, axis=-1, keepdims=True)

        total = lax.fori_loop(0, n_tp, one, jnp.zeros((branch_rows, 1), f32))
        scale = lax.rsqrt(total / width + norm_eps)

        def two(q, _):
            mixer_out[:, colsl(q)] = (proj[:, colsl(q)] * scale * out_gain[:, colsl(q)]).astype(bf16)
            return 0

        lax.fori_loop(0, n_tp, two, 0)

    def step(s, _):
        @pl.when(s < nz)
        def _():
            @pl.when(s == 0)
            def _():
                own_arr = remote(x_own, xg.at[mate], s_p.at[0], r_p.at[0], mate, j)
                own_arr.wait_recv()

            @pl.when(s > 0)
            def _():
                p_arrival(s).wait_recv()

            @pl.when(s + 2 < nz)
            def _():
                forward(s + 2)

            normed(src_ep(s), 0)
            normed(src_mate(s), rows)
            hidden_part()

        @pl.when((s > 0) & (s <= nz))
        def _():
            stage_two(s - 1)

        @pl.when(s < nz)
        def _():
            @pl.when(s == 0)
            def _():
                loads[2].wait()

            down_part(s)
            mate_sum(s).start()

            @pl.when(s + 1 < nz)
            def _():
                to_mate(s + 1)

        @pl.when(s == 0)
        def _():
            for t in range(1, n_tp):
                ow_arrival(t).wait_recv()
                owp_copy(t).start()

        @pl.when(s == nz)
        def _():
            project()

        @pl.when(s > 1)
        def _():
            stage_three(s - 2)

        return 0

    lax.fori_loop(0, nz + 2, step, 0)

    acc = facc[...]
    for d in range(1, nz):
        f_copy(d).wait_recv()
        acc = acc + frecv[d].astype(f32)
    expert_out[...] = acc.astype(bf16)

    own_p.wait_send()
    rim_copy.wait_send()
    for d in range(1, n_ep):
        w_copy(d).wait_send()
    for t in range(1, n_tp):
        ow_copy(t).wait_send()
        owp_copy(t).wait_send()

    def drain(s, _):
        mate_sum(s).wait_send()
        for t in range(1, n_tp):
            t_copy(s, t).wait_send()

        @pl.when(s > 0)
        def _():
            z_copy(s).wait_send()
            p_copy(s).wait_send()
            f_copy(s).wait_send()
            for t in range(1, n_tp):
                x_copy(s, t).wait_send()

        return 0

    lax.fori_loop(0, nz, drain, 0)


def per_device(
    n_ep, n_tp,
    branch_in, pool_weight, group_gain, out_weight, out_gain,
    ffn_input, ffn_gain, routes, route_weight, gate_weight, up_weight, down_weight,
):
    rows, width = ffn_input.shape
    nz = n_ep // 2
    cols = width // n_tp
    hidden = gate_weight.shape[2]
    branch_rows, branch_width = branch_in.shape
    named = routes[None, :, :] == jnp.arange(n_ep, dtype=jnp.int32)[:, None, None]
    w_own = jnp.sum(jnp.where(named, route_weight[None, :, :], 0.0), axis=2)
    vm = pl.BlockSpec(memory_space=pltpu.VMEM)
    anyspace = pl.BlockSpec(memory_space=pl.ANY)
    dma = pltpu.SemaphoreType.DMA
    return pl.pallas_call(
        functools.partial(kernel, n_ep, n_tp),
        out_shape=(
            jax.ShapeDtypeStruct((branch_rows, width), bf16),
            jax.ShapeDtypeStruct((rows, cols), bf16),
        ),
        in_specs=[vm] * 8 + [anyspace] * 3,
        out_specs=(vm, vm),
        scratch_shapes=[
            pltpu.VMEM((width, hidden), bf16),
            pltpu.VMEM((width, hidden), bf16),
            pltpu.VMEM((hidden, width), bf16),
            pltpu.VMEM((n_ep, rows, width), bf16),
            pltpu.VMEM((n_ep, n_ep, rows), f32),
            pltpu.VMEM((rim_rows, branch_width), bf16),
            pltpu.VMEM((n_tp, branch_width, cols), bf16),
            pltpu.VMEM((2 * rows, width), bf16),
            pltpu.VMEM((2 * rows, hidden), bf16),
            pltpu.VMEM((branch_rows, branch_width), bf16),
            pltpu.VMEM((branch_rows, width), f32),
            pltpu.VMEM((2, rows, width), f32),
            pltpu.VMEM((nz, rows, width), bf16),
            pltpu.VMEM((nz, rows, width), bf16),
            pltpu.VMEM((nz, rows, width), bf16),
            pltpu.VMEM((nz, n_tp, rows, cols), bf16),
            pltpu.VMEM((nz, rows, cols), bf16),
            pltpu.VMEM((nz, rows, cols), bf16),
            pltpu.VMEM((rows, cols), f32),
            dma((6,)),
            dma((nz,)), dma((nz,)),
            dma((nz, n_tp)), dma((nz, n_tp)),
            dma((nz,)), dma((nz,)),
            dma((n_ep,)), dma((n_ep,)),
            dma, dma,
            dma((n_tp,)), dma((n_tp,)),
            dma((n_tp,)), dma((n_tp,)),
            dma((nz,)), dma((nz,)),
            dma((nz, n_tp)), dma((nz, n_tp)),
            dma((nz,)), dma((nz,)),
        ],
        compiler_params=pltpu.CompilerParams(
            collective_id=0, has_side_effects=True, vmem_limit_bytes=67043328
        ),
    )(
        branch_in, pool_weight, group_gain.reshape(1, -1), out_weight, out_gain.reshape(1, -1),
        ffn_input, ffn_gain.reshape(1, -1), w_own, gate_weight, up_weight, down_weight,
    )


def solution(mesh):
    in_specs = (
        P(("ep", "tp"), None),
        P(),
        P(),
        P(None, "tp"),
        P(),
        P("ep", None),
        P(),
        P("ep", None),
        P("ep", None),
        P("ep", None, "tp"),
        P("ep", None, "tp"),
        P("ep", "tp", None),
    )
    out_specs = (P(("ep", "tp"), None), P("ep", "tp"))
    return jax.shard_map(
        functools.partial(per_device, mesh.shape["ep"], mesh.shape["tp"]),
        mesh=mesh, in_specs=in_specs, out_specs=out_specs, check_vma=False,
    )
```

```python
import functools
import jax
import jax.numpy as jnp
from jax import lax
from jax.experimental import pallas as pl
from jax.experimental.pallas import tpu as pltpu
from jax.sharding import PartitionSpec as P

pool_windows = (2, 4, 8, 16)
rim_rows = 16
norm_eps = 1e-06
clamp_limit = 7.0
sigmoid_slope = 1.702
MESH = pl.DeviceIdType.MESH
f32 = jnp.float32
bf16 = jnp.bfloat16


def rms_scale(values, gain):
    return values * lax.rsqrt(jnp.mean(values * values, axis=-1, keepdims=True) + norm_eps) * gain


def kernel(
    n_ep, n_tp,
    branch, pool_w, group_gain, out_w, out_gain, x_own, ffn_gain, w_own, gate_h, up_h, down_h,
    mixer_out, expert_out,
    gate, up, down, xg, wg, rim, ow, hid, mixed, proj,
    pown, psend, precv, tsend, trecv, fsend, frecv, facc,
    local_sem, s_z, r_z, s_x, r_x, s_p, r_p, s_w, r_w, s_rim, r_rim,
    s_ow, r_ow, s_owp, r_owp, s_ps, r_ps, s_t, r_t, s_f, r_f,
):
    e = lax.axis_index("ep")
    j = lax.axis_index("tp")
    nz = n_ep // 2
    z = e // 2
    c = e % 2
    rows, width = x_own.shape
    cols = width // n_tp
    mate = z * 2 + (1 - c)
    last = (j == n_tp - 1).astype(jnp.int32)
    first = (j == 0).astype(jnp.int32)
    nxt = ((e + last) % n_ep, (j + 1) % n_tp)
    prv = ((e - first + n_ep) % n_ep, (j - 1 + n_tp) % n_tp)

    def colsl(q):
        return pl.ds(pl.multiple_of(q * cols, cols), cols)

    def remote(src, dst, ssem, rsem, ep, tp):
        return pltpu.make_async_remote_copy(
            src_ref=src, dst_ref=dst, send_sem=ssem, recv_sem=rsem,
            device_id=(ep, tp), device_id_type=MESH,
        )

    def ep_at(d):
        return (z + d) % nz * 2 + c

    def src_ep(d):
        return (z - d + nz) % nz * 2 + c

    def src_mate(d):
        return (z - d + nz) % nz * 2 + (1 - c)

    def tp_at(t):
        return (j + t) % n_tp

    loads = [
        pltpu.make_async_copy(gate_h.at[0], gate, local_sem.at[0]),
        pltpu.make_async_copy(up_h.at[0], up, local_sem.at[1]),
        pltpu.make_async_copy(down_h.at[0], down, local_sem.at[2]),
    ]
    own_w = pltpu.make_async_copy(w_own, wg.at[e], local_sem.at[4])
    own_ow = pltpu.make_async_copy(out_w, ow.at[j], local_sem.at[5])
    own_w.start()
    own_ow.start()
    for load in loads:
        load.start()

    barrier = pltpu.get_barrier_semaphore()
    for d in range(1, n_ep):
        pl.semaphore_signal(barrier, inc=1, device_id=((e + d) % n_ep, j), device_id_type=MESH)
    for t in range(1, n_tp):
        pl.semaphore_signal(barrier, inc=1, device_id=(e, tp_at(t)), device_id_type=MESH)
    pl.semaphore_signal(barrier, inc=1, device_id=nxt, device_id_type=MESH)
    pl.semaphore_signal(barrier, inc=1, device_id=prv, device_id_type=MESH)

    chunk = 16

    def norm_rows(i, _):
        r = pl.ds(pl.multiple_of(i * chunk, chunk), chunk)
        xg[e, r, :] = rms_scale(x_own[r, :].astype(f32), ffn_gain[...]).astype(bf16)
        return 0

    lax.fori_loop(0, rows // chunk, norm_rows, 0)
    pl.semaphore_wait(barrier, n_ep - 1 + n_tp - 1 + 2)

    def z_copy(d):
        return remote(
            xg.at[e, :, colsl(j)], xg.at[e, :, colsl(j)], s_z.at[d], r_z.at[d], ep_at(d), j
        )

    def z_arrival(d):
        view = xg.at[src_ep(d), :, colsl(j)]
        return remote(view, view, s_z.at[d], r_z.at[d], ep_at(d), j)

    def x_copy(d, t):
        view = xg.at[src_ep(d), :, colsl(j)]
        return remote(view, view, s_x.at[d, t], r_x.at[d, t], e, tp_at(t))

    def x_arrival(d, t):
        view = xg.at[src_ep(d), :, colsl(tp_at(n_tp - t))]
        return remote(view, view, s_x.at[d, t], r_x.at[d, t], e, tp_at(t))

    def p_copy(d):
        view = xg.at[src_ep(d)]
        return remote(view, view, s_p.at[d], r_p.at[d], mate, j)

    def p_arrival(d):
        view = xg.at[src_mate(d)]
        return remote(view, view, s_p.at[d], r_p.at[d], mate, j)

    own_p = remote(xg.at[e], xg.at[e], s_p.at[0], r_p.at[0], mate, j)
    half = out_w.shape[0] // 2
    my_half = pl.ds(pl.multiple_of(c * half, half), half)
    mate_half = pl.ds(pl.multiple_of((1 - c) * half, half), half)

    def w_copy(d):
        return remote(w_own, wg.at[e], s_w.at[d], r_w.at[d], (e + d) % n_ep, j)

    def w_arrival(d):
        return remote(w_own, wg.at[(e - d + n_ep) % n_ep], s_w.at[d], r_w.at[d], (e + d) % n_ep, j)

    def ow_copy(t):
        return remote(
            out_w.at[my_half], ow.at[j, my_half], s_ow.at[t], r_ow.at[t], e, tp_at(t)
        )

    def ow_arrival(t):
        view = ow.at[tp_at(n_tp - t), my_half]
        return remote(view, view, s_ow.at[t], r_ow.at[t], e, tp_at(t))

    def owp_copy(t):
        view = ow.at[tp_at(n_tp - t), my_half]
        return remote(view, view, s_owp.at[t], r_owp.at[t], mate, j)

    def owp_arrival(t):
        view = ow.at[tp_at(n_tp - t), mate_half]
        return remote(view, view, s_owp.at[t], r_owp.at[t], mate, j)

    rim_copy = remote(
        branch.at[pl.ds(branch.shape[0] - rim_rows, rim_rows)], rim, s_rim, r_rim, nxt[0], nxt[1]
    )

    for d in range(1, nz):
        z_copy(d).start()
    own_p.start()
    rim_copy.start()
    for d in range(1, n_ep):
        w_copy(d).start()
    for t in range(1, n_tp):
        ow_copy(t).start()

    rim_copy.wait_recv()
    branch_rows = branch.shape[0]
    chans = branch.shape[1] // len(pool_windows)
    first_row = (e * n_tp + j) * branch_rows
    positions = first_row + lax.broadcasted_iota(jnp.int32, (branch_rows, 1), 0)
    total = jnp.zeros((branch_rows, 1), f32)
    for g, window in enumerate(pool_windows):
        lanes = slice(g * chans, (g + 1) * chans)
        here = branch[:, lanes].astype(f32)
        edge = jnp.where(first_row == 0, 0.0, rim[:, lanes].astype(f32))
        wide = jnp.concatenate([edge, here], axis=0)
        reach = 1
        while reach < window:
            wide = wide + pltpu.roll(wide, reach, 0)
            reach *= 2
        counts = jnp.minimum(window, positions + 1).astype(f32)
        pooled = (wide[rim_rows:] / counts - here).astype(bf16)
        part = jnp.dot(pooled, pool_w[g], preferred_element_type=f32)
        proj[:, lanes] = part
        total = total + jnp.sum(part * part, axis=-1, keepdims=True)
    scale = lax.rsqrt(total / branch.shape[1] + norm_eps)
    mixed[...] = (proj[:, : branch.shape[1]] * scale * group_gain[...]).astype(bf16)

    def forward(d):
        z_arrival(d).wait_recv()
        for t in range(1, n_tp):
            x_copy(d, t).start()

    def to_mate(d):
        for t in range(1, n_tp):
            x_arrival(d, t).wait_recv()
        p_copy(d).start()

    if nz > 1:
        forward(1)
    own_w.wait()
    own_ow.wait()
    for d in range(1, n_ep):
        w_arrival(d).wait_recv()
    for load in loads[:2]:
        load.wait()

    diagonal = lax.broadcasted_iota(jnp.int32, (rows, rows), 0) == lax.broadcasted_iota(
        jnp.int32, (rows, rows), 1
    )

    def row_weights(block):
        line = wg[block, pl.ds(e, 1), :]
        return jnp.sum(jnp.where(diagonal, line, 0.0), axis=1, keepdims=True)

    step_f = min(512, gate.shape[1])

    def hidden_part(s):
        def one(n, _):
            span = pl.ds(pl.multiple_of(n * step_f, step_f), step_f)
            both = jnp.concatenate([xg[src_ep(s)], xg[src_mate(s)]], axis=0)
            g = jnp.dot(both, gate[:, span], preferred_element_type=f32)
            u = jnp.dot(both, up[:, span], preferred_element_type=f32)
            g = jnp.minimum(g, clamp_limit)
            u = jnp.clip(u, -clamp_limit, clamp_limit)
            hid[:, span] = ((u + 1.0) * g * jax.nn.sigmoid(sigmoid_slope * g)).astype(bf16)
            return 0

        lax.fori_loop(0, gate.shape[1] // step_f, one, 0)

    step_d = min(512, width)

    def down_part(s):
        mine = row_weights(src_ep(s))
        theirs = row_weights(src_mate(s))

        def one(q, _):
            span = pl.ds(pl.multiple_of(q * step_d, step_d), step_d)
            y = jnp.dot(hid[...], down[:, span], preferred_element_type=f32)
            pown[s % 2, :, span] = y[:rows] * mine
            psend[s, :, span] = (y[rows:] * theirs).astype(bf16)
            return 0

        lax.fori_loop(0, width // step_d, one, 0)

    def mate_sum(s):
        return remote(psend.at[s], precv.at[s], s_ps.at[s], r_ps.at[s], mate, j)

    def t_copy(s, t):
        return remote(
            tsend.at[s, :, colsl(tp_at(t))], trecv.at[s, t], s_t.at[s, t], r_t.at[s, t], e, tp_at(t)
        )

    def f_copy(s):
        return remote(fsend.at[s], frecv.at[s], s_f.at[s], r_f.at[s], src_ep(s), j)

    def stage_two(s):
        mate_sum(s).wait_recv()

        def one(i, _):
            r = pl.ds(pl.multiple_of(i * chunk, chunk), chunk)
            tsend[s, r, :] = (pown[s % 2, r, :] + precv[s, r, :].astype(f32)).astype(bf16)
            return 0

        lax.fori_loop(0, rows // chunk, one, 0)
        for t in range(1, n_tp):
            t_copy(s, t).start()

    def stage_three(s):
        for t in range(1, n_tp):
            t_copy(s, t).wait_recv()
        acc = tsend[s, :, colsl(j)].astype(f32)
        for t in range(1, n_tp):
            acc = acc + trecv[s, t].astype(f32)

        @pl.when(s == 0)
        def _():
            facc[...] = acc

        @pl.when(s > 0)
        def _():
            fsend[s] = acc.astype(bf16)
            f_copy(s).start()

    def project():
        for t in range(1, n_tp):
            owp_arrival(t).wait_recv()

        def one(q, total):
            part = jnp.dot(mixed[...], ow[q], preferred_element_type=f32)
            proj[:, colsl(q)] = part
            return total + jnp.sum(part * part, axis=-1, keepdims=True)

        total = lax.fori_loop(0, n_tp, one, jnp.zeros((branch_rows, 1), f32))
        scale = lax.rsqrt(total / width + norm_eps)

        def two(q, _):
            mixer_out[:, colsl(q)] = (proj[:, colsl(q)] * scale * out_gain[:, colsl(q)]).astype(bf16)
            return 0

        lax.fori_loop(0, n_tp, two, 0)

    def step(s, _):
        @pl.when(s < nz)
        def _():
            @pl.when(s == 0)
            def _():
                own_arr = remote(xg.at[mate], xg.at[mate], s_p.at[0], r_p.at[0], mate, j)
                own_arr.wait_recv()

            @pl.when(s > 0)
            def _():
                p_arrival(s).wait_recv()

            @pl.when(s + 2 < nz)
            def _():
                forward(s + 2)

            hidden_part(s)

        @pl.when((s > 0) & (s <= nz))
        def _():
            stage_two(s - 1)

        @pl.when(s < nz)
        def _():
            @pl.when(s == 0)
            def _():
                loads[2].wait()

            down_part(s)
            mate_sum(s).start()

            @pl.when(s + 1 < nz)
            def _():
                to_mate(s + 1)

        @pl.when(s == 0)
        def _():
            for t in range(1, n_tp):
                ow_arrival(t).wait_recv()
                owp_copy(t).start()

        @pl.when(s == nz)
        def _():
            project()

        @pl.when(s > 1)
        def _():
            stage_three(s - 2)

        return 0

    lax.fori_loop(0, nz + 2, step, 0)

    acc = facc[...]
    for d in range(1, nz):
        f_copy(d).wait_recv()
        acc = acc + frecv[d].astype(f32)
    expert_out[...] = acc.astype(bf16)

    own_p.wait_send()
    rim_copy.wait_send()
    for d in range(1, n_ep):
        w_copy(d).wait_send()
    for t in range(1, n_tp):
        ow_copy(t).wait_send()
        owp_copy(t).wait_send()

    def drain(s, _):
        mate_sum(s).wait_send()
        for t in range(1, n_tp):
            t_copy(s, t).wait_send()

        @pl.when(s > 0)
        def _():
            z_copy(s).wait_send()
            p_copy(s).wait_send()
            f_copy(s).wait_send()
            for t in range(1, n_tp):
                x_copy(s, t).wait_send()

        return 0

    lax.fori_loop(0, nz, drain, 0)


def per_device(
    n_ep, n_tp,
    branch_in, pool_weight, group_gain, out_weight, out_gain,
    ffn_input, ffn_gain, routes, route_weight, gate_weight, up_weight, down_weight,
):
    rows, width = ffn_input.shape
    nz = n_ep // 2
    cols = width // n_tp
    hidden = gate_weight.shape[2]
    branch_rows, branch_width = branch_in.shape
    named = routes[None, :, :] == jnp.arange(n_ep, dtype=jnp.int32)[:, None, None]
    w_own = jnp.sum(jnp.where(named, route_weight[None, :, :], 0.0), axis=2)
    vm = pl.BlockSpec(memory_space=pltpu.VMEM)
    anyspace = pl.BlockSpec(memory_space=pl.ANY)
    dma = pltpu.SemaphoreType.DMA
    return pl.pallas_call(
        functools.partial(kernel, n_ep, n_tp),
        out_shape=(
            jax.ShapeDtypeStruct((branch_rows, width), bf16),
            jax.ShapeDtypeStruct((rows, cols), bf16),
        ),
        in_specs=[vm] * 8 + [anyspace] * 3,
        out_specs=(vm, vm),
        scratch_shapes=[
            pltpu.VMEM((width, hidden), bf16),
            pltpu.VMEM((width, hidden), bf16),
            pltpu.VMEM((hidden, width), bf16),
            pltpu.VMEM((n_ep, rows, width), bf16),
            pltpu.VMEM((n_ep, n_ep, rows), f32),
            pltpu.VMEM((rim_rows, branch_width), bf16),
            pltpu.VMEM((n_tp, branch_width, cols), bf16),
            pltpu.VMEM((2 * rows, hidden), bf16),
            pltpu.VMEM((branch_rows, branch_width), bf16),
            pltpu.VMEM((branch_rows, width), f32),
            pltpu.VMEM((2, rows, width), f32),
            pltpu.VMEM((nz, rows, width), bf16),
            pltpu.VMEM((nz, rows, width), bf16),
            pltpu.VMEM((nz, rows, width), bf16),
            pltpu.VMEM((nz, n_tp, rows, cols), bf16),
            pltpu.VMEM((nz, rows, cols), bf16),
            pltpu.VMEM((nz, rows, cols), bf16),
            pltpu.VMEM((rows, cols), f32),
            dma((6,)),
            dma((nz,)), dma((nz,)),
            dma((nz, n_tp)), dma((nz, n_tp)),
            dma((nz,)), dma((nz,)),
            dma((n_ep,)), dma((n_ep,)),
            dma, dma,
            dma((n_tp,)), dma((n_tp,)),
            dma((n_tp,)), dma((n_tp,)),
            dma((nz,)), dma((nz,)),
            dma((nz, n_tp)), dma((nz, n_tp)),
            dma((nz,)), dma((nz,)),
        ],
        compiler_params=pltpu.CompilerParams(
            collective_id=0, has_side_effects=True, vmem_limit_bytes=67043328
        ),
    )(
        branch_in, pool_weight, group_gain.reshape(1, -1), out_weight, out_gain.reshape(1, -1),
        ffn_input, ffn_gain.reshape(1, -1), w_own, gate_weight, up_weight, down_weight,
    )


def solution(mesh):
    in_specs = (
        P(("ep", "tp"), None),
        P(),
        P(),
        P(None, "tp"),
        P(),
        P("ep", None),
        P(),
        P("ep", None),
        P("ep", None),
        P("ep", None, "tp"),
        P("ep", None, "tp"),
        P("ep", "tp", None),
    )
    out_specs = (P(("ep", "tp"), None), P("ep", "tp"))
    return jax.shard_map(
        functools.partial(per_device, mesh.shape["ep"], mesh.shape["tp"]),
        mesh=mesh, in_specs=in_specs, out_specs=out_specs, check_vma=False,
    )
```
